32 devices in a mesh: ep: 8 (over z, y), tp: 4 (over x, core).
Axes of the slice: x: 2, y: 2, z: 4, core: 2. Of those that a mesh axis runs over, the one named last changes fastest.
Arguments:
- queries: bfloat16 [2048, 1536], P('ep', 'tp'), may hold values from -6 to 6
- kv_latent: bfloat16 [2048, 512], P('ep'), may hold values from -6 to 6
- rope_key: bfloat16 [2048, 64], P('ep'), may hold values from -6 to 6
- latent_gain: float32 [512], replicated, may hold values from 0.1 to 1.9
- w_key_up: bfloat16 [512, 1024], P(None, 'tp'), may hold values from -0.25 to 0.25
- w_value_up: bfloat16 [512, 1024], P(None, 'tp'), may hold values from -0.25 to 0.25
- query_gain: float32 [192], replicated, may hold values from 0.1 to 1.9
- key_gain: float32 [128], replicated, may hold values from 0.1 to 1.9
- rope_gain: float32 [64], replicated, may hold values from 0.1 to 1.9
- out_gain: float32 [128], replicated, may hold values from 0.1 to 1.9
- moe_tokens: bfloat16 [2048, 2048], P('ep'), may hold values from -6 to 6
- moe_gain: float32 [2048], replicated, may hold values from 0.1 to 1.9
- routes: int32 [2048, 2], P('ep'), may hold values from 0 to 7, all different within a row; in each aligned block of 64 rows (0 to 63, 64 to 127, ...) at most 24 rows name the same one
- route_weights: float32 [2048, 2], P('ep'), may hold values from 0.25 to 1
- w_gate: bfloat16 [8, 2048, 3584], P('ep', None, 'tp'), may hold values from -0.125 to 0.125
- w_up: bfloat16 [8, 2048, 3584], P('ep', None, 'tp'), may hold values from -0.125 to 0.125
- w_down: bfloat16 [8, 3584, 2048], P('ep', 'tp'), may hold values from -0.09375 to 0.09375
Outputs:
- attended: bfloat16 [2048, 1024], P('ep', 'tp')
- moe_out: bfloat16 [2048, 2048], P(('ep', 'tp'))
The draws below stay inside these ranges and needn't reach their ends.
Inputs may be any that keep to these rules, and one draw needn't show every extreme that they name: `routes`: each row names 2 different experts of 0 to 7; in each aligned block of 64 rows no expert is named by more than 24 rows, and in some block one expert is named by exactly 24.
All inputs are finite; a program needn't handle non-finite values.
Results may differ from the reference program's by a relative error of at most 0.0071.
Values may be sent and summed in bfloat16 or wider, within the bound.
A program may use at most 128 MiB of HBM per device.

```python
import math
import jax
import jax.numpy as jnp
import numpy as np
from jax import lax

D = 2048
HEADS = 8
NOPE = 128
ROPE_DIM = 64
VHEAD = 128
LATENT = 512
FF = 3584
TOP = 2
EXPERTS = 8
SEQ = 2048
MOE_ROWS = 2048
Q_ROWS = 64
CAP = 24


def shard_levels(stream_key, extent, shards, least, largest):
    def one(dim, parts):
        heights = jax.random.uniform(jax.random.fold_in(jax.random.fold_in(stream_key, 6), dim), (parts,), jnp.float32, least / len(shards), largest / len(shards))
        return jnp.repeat(jnp.exp(heights), extent[dim] // parts).reshape((-1,) + (1,) * (len(extent) - dim - 1))

    level = one(*shards[0])
    for cut in shards[1:]:
        level = level * one(*cut)
    return level


def assign_block(key, own, number, rows, count, top, bound, lean):
    order = jax.random.permutation(key, count)
    heavy_load, ordinary = portions_of(count, rows * top, bound, lean, True), portions_of(count, rows * top, bound, lean, False)
    places = jnp.arange(count)

    def named(tallies, offset_by):
        used = int((tallies > 0).sum())
        fixed = max(1, used // 4)
        shifted = fixed + (places - fixed + offset_by * (used - fixed)) % max(1, count - fixed)
        return jnp.zeros((count,), jnp.int32).at[order[jnp.where(places < fixed, places, shifted)]].set(jnp.asarray(tallies, jnp.int32))

    tallies = jnp.where(number % 4 == 0, named(heavy_load, number // 4), named(ordinary, number - number // 4 - 1))
    mixed = jax.random.permutation(jax.random.fold_in(own, 3), count)
    giver, receiver = mixed[0:count // 2 * 2:2], mixed[1:count // 2 * 2:2]
    margin = jnp.minimum(tallies[giver] - 1, bound - tallies[receiver]) // 2
    margin = jnp.where((giver == order[0]) | (receiver == order[0]) | (tallies[receiver] == 0), 0, jnp.maximum(margin, 0))
    shifted = jax.random.randint(jax.random.fold_in(own, 4), (count // 2,), 0, 1 << 20) % (margin + 1)
    tallies = tallies.at[giver].add(-shifted).at[receiver].add(shifted)
    labels = jnp.searchsorted(jnp.cumsum(tallies), jnp.arange(rows * top), side="right").astype(jnp.int32)
    table = labels.reshape(top, rows).T
    table = table[jax.random.permutation(jax.random.fold_in(own, 1), rows)]
    offset_by = jax.random.randint(jax.random.fold_in(own, 2), (rows, 1), 0, top)
    return jnp.take_along_axis(table, (jnp.arange(top)[None, :] + offset_by) % top, axis=1)


def portions_of(number_of, total, most, skew, full):
    portions = [(1 << 20) // math.isqrt(standing ** skew) + 1 for standing in range(1, number_of + 1)]
    largest = most if full else min(most, max(-(-total // number_of), total * portions[0] // sum(portions)))
    least = 1 if total - largest >= number_of - 1 else 0
    given, surplus = [largest] + [least] * (number_of - 1), total - largest - least * (number_of - 1)
    while surplus > 0:
        movable = [i for i in range(1, number_of) if given[i] < largest] or [i for i in range(1, number_of) if given[i] < most]
        mass, remaining = sum([portions[i] for i in movable]), surplus
        for i in movable:
            addition = min(most - given[i], max(1, remaining * portions[i] // mass), surplus)
            given[i] = given[i] + addition
            surplus = surplus - addition
    return np.array(given)


def scatter_about(stream_key, dims, scale, limit, shards=(), held_as=jnp.bfloat16):
    drawn = scale * jax.random.normal(stream_key, dims, jnp.float32)
    if shards:
        drawn = drawn * shard_levels(stream_key, dims, shards, -0.22, 0.18)
    return jnp.clip(drawn, -limit, limit).astype(held_as)


def setup_inputs(seed: int = 0) -> dict:
    streams_of = jax.random.split(jax.random.key(seed), 18)
    queries = scatter_about(streams_of[0], (SEQ, HEADS * (NOPE + ROPE_DIM)), 1.0, 6.0, ((0, 8), (1, 4)))
    kv_latent = scatter_about(streams_of[1], (SEQ, LATENT), 1.0, 6.0, ((0, 8),))
    rope_key = scatter_about(streams_of[2], (SEQ, ROPE_DIM), 1.0, 6.0, ((0, 8),))
    latent_gain = jnp.clip(1.0 + 0.18 * jax.random.normal(streams_of[3], (LATENT,), jnp.float32), 0.1, 1.9)
    w_key_up = scatter_about(streams_of[4], (LATENT, HEADS * NOPE), LATENT ** -0.5, 0.25, ((1, 4),))
    w_value_up = scatter_about(streams_of[5], (LATENT, HEADS * VHEAD), LATENT ** -0.5, 0.25, ((1, 4),))
    query_gain = jnp.clip(1.0 + 0.18 * jax.random.normal(streams_of[6], (NOPE + ROPE_DIM,), jnp.float32), 0.1, 1.9)
    key_gain = jnp.clip(1.0 + 0.18 * jax.random.normal(streams_of[7], (NOPE,), jnp.float32), 0.1, 1.9)
    rope_gain = jnp.clip(1.0 + 0.18 * jax.random.normal(streams_of[8], (ROPE_DIM,), jnp.float32), 0.1, 1.9)
    out_gain = jnp.clip(1.0 + 0.18 * jax.random.normal(streams_of[9], (VHEAD,), jnp.float32), 0.1, 1.9)
    moe_tokens = scatter_about(streams_of[10], (MOE_ROWS, D), 1.0, 6.0, ((0, 8),))
    moe_gain = jnp.clip(1.0 + 0.18 * jax.random.normal(streams_of[11], (D,), jnp.float32), 0.1, 1.9)
    routes_keys = jax.random.split(jax.random.fold_in(streams_of[12], 1), MOE_ROWS // Q_ROWS)
    routes_turns = jax.random.permutation(jax.random.fold_in(streams_of[12], 3), MOE_ROWS // Q_ROWS)
    routes = jax.vmap(lambda own, number: assign_block(jax.random.fold_in(streams_of[12], 2), own, number, Q_ROWS, EXPERTS, TOP, CAP, 1))(routes_keys, routes_turns).reshape((MOE_ROWS, TOP))
    route_weights = jnp.clip(0.25 + 0.75 * jax.random.uniform(streams_of[13], (MOE_ROWS, TOP), jnp.float32) ** shard_levels(streams_of[13], (MOE_ROWS, TOP), ((0, 8),), -0.2, 0.2), 0.25, 1.0)
    w_gate = scatter_about(streams_of[14], (EXPERTS, D, FF), D ** -0.5, 0.125, ((0, 8), (2, 4)))
    w_up = scatter_about(streams_of[15], (EXPERTS, D, FF), D ** -0.5, 0.125, ((0, 8), (2, 4)))
    w_down = scatter_about(streams_of[16], (EXPERTS, FF, D), FF ** -0.5, 0.09375, ((0, 8), (1, 4)))
    return {"queries": queries, "kv_latent": kv_latent, "rope_key": rope_key, "latent_gain": latent_gain, "w_key_up": w_key_up, "w_value_up": w_value_up, "query_gain": query_gain, "key_gain": key_gain, "rope_gain": rope_gain, "out_gain": out_gain, "moe_tokens": moe_tokens, "moe_gain": moe_gain, "routes": routes, "route_weights": route_weights, "w_gate": w_gate, "w_up": w_up, "w_down": w_down}


EPS = 1e-06
THETA = 500000.0

def rms_norm(values, norm_gain):
    return values * lax.rsqrt(lax.optimization_barrier(jnp.mean(values * values, axis=-1, keepdims=True)) + EPS) * norm_gain

def rounded(values):
    return lax.optimization_barrier(values.astype(jnp.bfloat16))

def rope_tables(positions, rope_dim):
    freqs = 1.0 / THETA ** (jnp.arange(0, rope_dim, 2, dtype=jnp.float32) / rope_dim)
    angles = positions.astype(jnp.float32)[:, None] * freqs[None, :]
    return (jnp.cos(angles), jnp.sin(angles))

def rotate(values, rot_cos, rot_sin):
    half_dim = values.shape[-1] // 2
    first_half = values[..., :half_dim]
    second_half = values[..., half_dim:]
    return jnp.concatenate([first_half * rot_cos - second_half * rot_sin, second_half * rot_cos + first_half * rot_sin], axis=-1)

def attention(queries, kv_latent, rope_key, latent_gain, w_key_up, w_value_up, query_gain, key_gain, rope_gain, out_gain):
    seq_len = queries.shape[0]
    positions = jnp.arange(seq_len, dtype=jnp.int32)
    rot_cos, rot_sin = rope_tables(positions, ROPE_DIM)
    latent = rounded(rms_norm(kv_latent.astype(jnp.float32), latent_gain))
    key_nope = jnp.dot(latent, w_key_up, preferred_element_type=jnp.float32).reshape(seq_len, HEADS, NOPE)
    key_nope = rounded(rms_norm(key_nope, key_gain)).astype(jnp.float32)
    values = rounded(jnp.dot(latent, w_value_up, preferred_element_type=jnp.float32))
    values = values.astype(jnp.float32).reshape(seq_len, HEADS, VHEAD)
    rot_key = rounded(rotate(rms_norm(rope_key.astype(jnp.float32), rope_gain), rot_cos, rot_sin)).astype(jnp.float32)
    query = rms_norm(queries.astype(jnp.float32).reshape(seq_len, HEADS, NOPE + ROPE_DIM), query_gain)
    query_nope = rounded(query[..., :NOPE]).astype(jnp.float32)
    query_rope = rounded(rotate(query[..., NOPE:], rot_cos[:, None, :], rot_sin[:, None, :])).astype(jnp.float32)
    scale = (NOPE + ROPE_DIM) ** (-0.5)
    block_rows = math.gcd(seq_len, 512)

    def one_block(block_index):
        block_first = block_index * block_rows
        q_nope = lax.dynamic_slice_in_dim(query_nope, block_first, block_rows, 0)
        q_rope = lax.dynamic_slice_in_dim(query_rope, block_first, block_rows, 0)
        scores = (jnp.einsum('qhd,khd->hqk', q_nope, key_nope, precision=lax.Precision.HIGHEST) + jnp.einsum('qhr,kr->hqk', q_rope, rot_key, precision=lax.Precision.HIGHEST)) * scale
        query_pos = block_first + jnp.arange(block_rows, dtype=jnp.int32)
        visible = (query_pos[:, None] >= positions[None, :])[None]
        exp_scores = jnp.where(visible, jnp.exp(scores), 0.0)
        denominator = lax.optimization_barrier(jnp.sum(exp_scores, axis=-1))
        weighted = jnp.einsum('hqk,khd->qhd', rounded(exp_scores).astype(jnp.float32), values, precision=lax.Precision.HIGHEST)
        mixed = weighted / jnp.transpose(denominator)[:, :, None]
        return rms_norm(mixed, out_gain).astype(jnp.bfloat16).reshape(block_rows, HEADS * VHEAD)
    blocks = lax.map(one_block, jnp.arange(seq_len // block_rows, dtype=jnp.int32))
    return blocks.reshape(seq_len, HEADS * VHEAD)

def experts_layer(moe_tokens, moe_gain, routes, route_weights, w_gate, w_up, w_down):
    n_rows = moe_tokens.shape[0]
    normed = rounded(rms_norm(moe_tokens.astype(jnp.float32), moe_gain))
    n_blocks = n_rows // Q_ROWS
    assigned = Q_ROWS * TOP
    slot_count = EXPERTS * CAP
    chosen = routes.reshape(n_blocks, assigned)
    onehot = (chosen[..., None] == jnp.arange(EXPERTS, dtype=jnp.int32)).astype(jnp.int32)
    rank = lax.optimization_barrier(jnp.sum((jnp.cumsum(onehot, axis=1) - onehot) * onehot, axis=-1)).astype(jnp.int32)
    slots = chosen * CAP + rank
    row_ids = jnp.arange(n_blocks, dtype=jnp.int32)[:, None] * Q_ROWS + jnp.arange(assigned, dtype=jnp.int32)[None, :] // TOP
    slot_hit = (slots[..., None] == jnp.arange(slot_count, dtype=jnp.int32)).astype(jnp.int32)
    table = lax.optimization_barrier(jnp.sum(slot_hit * (row_ids[..., None] + 1), axis=1)) - 1
    table = jnp.where(table < 0, n_rows, table).astype(jnp.int32)
    padded = jnp.concatenate([normed, jnp.zeros((1, normed.shape[1]), jnp.bfloat16)], axis=0)

    def one_expert(expert):
        rows_used = lax.dynamic_slice_in_dim(table, expert * CAP, CAP, 1).reshape(-1)
        inputs = padded[rows_used]
        gate = jnp.dot(inputs, w_gate[expert], preferred_element_type=jnp.float32)
        upward = jnp.dot(inputs, w_up[expert], preferred_element_type=jnp.float32)
        hidden = (jax.nn.silu(gate) * upward).astype(jnp.bfloat16)
        return rounded(jnp.dot(hidden, w_down[expert], preferred_element_type=jnp.float32))
    outputs = lax.map(one_expert, jnp.arange(EXPERTS, dtype=jnp.int32))
    place = jnp.arange(n_blocks, dtype=jnp.int32)[:, None] * CAP + rank
    picked = outputs[chosen, place].astype(jnp.float32)
    scaled = picked * route_weights.reshape(n_blocks, assigned)[..., None]
    mixed = lax.optimization_barrier(jnp.sum(scaled.reshape(n_rows, TOP, picked.shape[-1]), axis=1))
    return mixed.astype(jnp.bfloat16)

def reference(queries, kv_latent, rope_key, latent_gain, w_key_up, w_value_up, query_gain, key_gain, rope_gain, out_gain, moe_tokens, moe_gain, routes, route_weights, w_gate, w_up, w_down):
    attended = attention(queries, kv_latent, rope_key, latent_gain, w_key_up, w_value_up, query_gain, key_gain, rope_gain, out_gain)
    moe_out = experts_layer(moe_tokens, moe_gain, routes, route_weights, w_gate, w_up, w_down)
    return (attended, moe_out)
```

```python
import functools
import math

import jax
import jax.numpy as jnp
from jax import lax
from jax.experimental import pallas as pl
from jax.experimental.pallas import tpu as pltpu
from jax.sharding import PartitionSpec as P

EPS = 1e-06
THETA = 500000.0


def rms_norm(values, norm_gain):
    return values * lax.rsqrt(jnp.mean(values * values, axis=-1, keepdims=True) + EPS) * norm_gain


def rope_tables(positions, rope_dim):
    freqs = 1.0 / THETA ** (jnp.arange(0, rope_dim, 2, dtype=jnp.float32) / rope_dim)
    angles = positions.astype(jnp.float32)[:, None] * freqs[None, :]
    return (jnp.cos(angles), jnp.sin(angles))


def rotate(values, rot_cos, rot_sin):
    half_dim = values.shape[-1] // 2
    first_half = values[..., :half_dim]
    second_half = values[..., half_dim:]
    return jnp.concatenate(
        [
            first_half * rot_cos - second_half * rot_sin,
            second_half * rot_cos + first_half * rot_sin,
        ],
        axis=-1,
    )

MESH = pl.DeviceIdType.MESH
VMEM = pltpu.VMEM


def remote(src, dst, send, recv, device):
    return pltpu.make_async_remote_copy(
        src_ref=src, dst_ref=dst, send_sem=send, recv_sem=recv, device_id=device, device_id_type=MESH
    )


def greet(me, quarter, n_ep, highs):
    high, low = quarter // 2, quarter % 2
    barrier = pltpu.get_barrier_semaphore()

    def hello(device):
        pl.semaphore_signal(barrier, inc=1, device_id=device, device_id_type=MESH)

    def hello_ep(step, carry):
        hello((lax.rem(me + step, n_ep), quarter))
        return carry

    lax.fori_loop(1, n_ep, hello_ep, 0)
    hello((me, high * 2 + 1 - low))
    for step in range(1, highs):
        hello((me, lax.rem(high + step, highs) * 2 + low))
    pl.semaphore_wait(barrier, n_ep - 1 + 1 + highs - 1)


def spread_kernel(
    n_ep, highs, rows_ref, lat_ref, arrived, lat_all,
    own_sem, ep_send, ep_recv, high_send, high_recv, low_send, low_recv,
):
    me, quarter = lax.axis_index("ep"), lax.axis_index("tp")
    high, low = quarter // 2, quarter % 2
    partner = (me, high * 2 + 1 - low)
    greet(me, quarter, n_ep, highs)
    payloads = (
        (lambda j: rows_ref.at[j], arrived),
        (lambda j: lat_ref, lat_all),
    )
    own = [
        pltpu.make_async_copy(outgoing(me), into.at[low, high, me], own_sem.at[p])
        for p, (outgoing, into) in enumerate(payloads)
    ]
    for copy in own:
        copy.start()

    def ep_copy(p, step):
        outgoing, into = payloads[p]
        j = lax.rem(me + step, n_ep)
        return remote(
            outgoing(j), into.at[low, high, me], ep_send.at[p, step], ep_recv.at[p, step], (j, quarter)
        )

    def ep_arrival(p, step):
        outgoing, into = payloads[p]
        j = lax.rem(me + n_ep - step, n_ep)
        return remote(
            outgoing(me), into.at[low, high, j], ep_send.at[p, step], ep_recv.at[p, step], (j, quarter)
        )

    def high_copy(p, step, hop):
        into = payloads[p][1]
        j = lax.rem(me + n_ep - step, n_ep)
        block = into.at[low, high, j]
        return remote(
            block, block, high_send.at[p, hop, step], high_recv.at[p, hop, step],
            (me, lax.rem(high + hop, highs) * 2 + low),
        )

    def high_arrival(p, step, hop):
        into = payloads[p][1]
        j = lax.rem(me + n_ep - step, n_ep)
        block = into.at[low, lax.rem(high + highs - hop, highs), j]
        return remote(
            block, block, high_send.at[p, hop, step], high_recv.at[p, hop, step],
            (me, lax.rem(high + hop, highs) * 2 + low),
        )

    def low_copy(p, step, hop, side):
        into = payloads[p][1]
        j = lax.rem(me + n_ep - step, n_ep)
        block = into.at[side, lax.rem(high + highs - hop, highs), j]
        return remote(block, block, low_send.at[p, hop, step], low_recv.at[p, hop, step], partner)

    def start_ep(step, carry, p):
        ep_copy(p, step).start()
        return carry

    def forward(step, carry, p):
        ep_arrival(p, step).wait_recv()
        for hop in range(1, highs):
            high_copy(p, step, hop).start()
        low_copy(p, step, 0, low).start()
        return carry

    def forward_low(step, carry, p):
        for hop in range(1, highs):
            high_arrival(p, step, hop).wait_recv()
            low_copy(p, step, hop, low).start()
        return carry

    def finish(step, carry, p):
        for hop in range(highs):
            low_copy(p, step, hop, 1 - low).wait_recv()
            low_copy(p, step, hop, low).wait_send()
        for hop in range(1, highs):
            high_copy(p, step, hop).wait_send()
        return carry

    def finish_ep(step, carry, p):
        ep_copy(p, step).wait_send()
        return carry

    for p in range(2):
        lax.fori_loop(1, n_ep, functools.partial(start_ep, p=p), 0)
    for p in range(2):
        own[p].wait()
        for hop in range(1, highs):
            high_copy(p, 0, hop).start()
        low_copy(p, 0, 0, low).start()
        lax.fori_loop(1, n_ep, functools.partial(forward, p=p), 0)
    for p in range(2):
        lax.fori_loop(0, n_ep, functools.partial(forward_low, p=p), 0)
    for p in range(2):
        lax.fori_loop(0, n_ep, functools.partial(finish, p=p), 0)
        lax.fori_loop(1, n_ep, functools.partial(finish_ep, p=p), 0)


def spread(rows, lat, quarters):
    n_ep, cap, model_dim = rows.shape
    highs = quarters // 2
    dma = pltpu.SemaphoreType.DMA
    return pl.pallas_call(
        functools.partial(spread_kernel, n_ep, highs),
        out_shape=(
            jax.ShapeDtypeStruct((2, highs, n_ep, cap, model_dim), rows.dtype),
            jax.ShapeDtypeStruct((2, highs, n_ep) + lat.shape, lat.dtype),
        ),
        in_specs=[pl.BlockSpec(memory_space=VMEM)] * 2,
        out_specs=(pl.BlockSpec(memory_space=VMEM),) * 2,
        scratch_shapes=[
            dma((2,)),
            dma((2, n_ep)),
            dma((2, n_ep)),
            dma((2, highs, n_ep)),
            dma((2, highs, n_ep)),
            dma((2, highs, n_ep)),
            dma((2, highs, n_ep)),
        ],
        compiler_params=pltpu.CompilerParams(
            collective_id=0, has_side_effects=True, vmem_limit_bytes=60 << 20
        ),
        name="spread",
    )(rows, lat)


def collect_kernel(
    n_ep, highs, part_ref, ret, low_buf, high_buf, sum_buf, final_buf,
    low_send, low_recv, high_send, high_recv, ep_send, ep_recv,
):
    me, quarter = lax.axis_index("ep"), lax.axis_index("tp")
    high, low = quarter // 2, quarter % 2
    partner = (me, high * 2 + 1 - low)
    greet(me, quarter, n_ep, highs)

    def low_copy(step):
        j = lax.rem(me + step, n_ep)
        return remote(
            part_ref.at[1 - low, j], low_buf.at[j], low_send.at[step], low_recv.at[step], partner
        )

    def high_copy(step, hop):
        j = lax.rem(me + step, n_ep)
        other = lax.rem(high + hop, highs)
        return remote(
            sum_buf.at[j, other], high_buf.at[hop, j], high_send.at[hop, step],
            high_recv.at[hop, step], (me, other * 2 + low),
        )

    def ep_copy(step):
        j = lax.rem(me + step, n_ep)
        return remote(final_buf.at[j], ret.at[me], ep_send.at[step], ep_recv.at[step], (j, quarter))

    def ep_arrival(step):
        j = lax.rem(me + n_ep - step, n_ep)
        return remote(final_buf.at[j], ret.at[j], ep_send.at[step], ep_recv.at[step], (j, quarter))

    def start_low(step, carry):
        low_copy(step).start()
        return carry

    def add_low(step, carry):
        low_copy(step).wait_recv()
        j = lax.rem(me + step, n_ep)
        sum_buf[j] = (
            part_ref[low, j].astype(jnp.float32) + low_buf[j].astype(jnp.float32)
        ).astype(jnp.bfloat16)
        for hop in range(1, highs):
            high_copy(step, hop).start()
        return carry

    def total(step):
        j = lax.rem(me + step, n_ep)
        value = part_ref[low, j, high].astype(jnp.float32) + low_buf[j, high].astype(jnp.float32)
        for hop in range(1, highs):
            high_copy(step, hop).wait_recv()
            value = value + high_buf[hop, j].astype(jnp.float32)
        return value.astype(jnp.bfloat16)

    def add_high(step, carry):
        final_buf[lax.rem(me + step, n_ep)] = total(step)
        ep_copy(step).start()
        return carry

    def finish(step, carry):
        ep_arrival(step).wait_recv()
        ep_copy(step).wait_send()
        return carry

    def finish_tp(step, carry):
        low_copy(step).wait_send()
        for hop in range(1, highs):
            high_copy(step, hop).wait_send()
        return carry

    lax.fori_loop(1, n_ep, start_low, 0)
    low_copy(0).start()
    lax.fori_loop(1, n_ep, add_low, 0)
    add_low(0, 0)
    lax.fori_loop(1, n_ep, add_high, 0)
    ret[me] = total(0)
    lax.fori_loop(1, n_ep, finish, 0)
    lax.fori_loop(0, n_ep, finish_tp, 0)


def collect(partial):
    _, n_ep, highs, cap, model_dim = partial.shape
    dma = pltpu.SemaphoreType.DMA
    kind = partial.dtype
    return pl.pallas_call(
        functools.partial(collect_kernel, n_ep, highs),
        out_shape=jax.ShapeDtypeStruct((n_ep, cap, model_dim), kind),
        in_specs=[pl.BlockSpec(memory_space=VMEM)],
        out_specs=pl.BlockSpec(memory_space=VMEM),
        scratch_shapes=[
            VMEM((n_ep, highs, cap, model_dim), kind),
            VMEM((highs, n_ep, cap, model_dim), kind),
            VMEM((n_ep, highs, cap, model_dim), kind),
            VMEM((n_ep, cap, model_dim), kind),
            dma((n_ep,)),
            dma((n_ep,)),
            dma((highs, n_ep)),
            dma((highs, n_ep)),
            dma((n_ep,)),
            dma((n_ep,)),
        ],
        compiler_params=pltpu.CompilerParams(
            collective_id=1, has_side_effects=True, vmem_limit_bytes=62 << 20
        ),
        name="collect",
    )(partial)


def attend_kernel(
    heads, nope_dim, value_dim, latent_dim, scale,
    lat_ref, wk_ref, wv_ref, qn_ref, qr_ref, kg_ref, og_ref, out_ref, acc, den,
):
    block = pl.program_id(0)
    block_rows = lat_ref.shape[0]
    tok_rows = qn_ref.shape[1]
    offset = lax.axis_index("ep") * tok_rows
    first = block * block_rows

    @pl.when(block == 0)
    def _():
        acc[...] = jnp.zeros_like(acc)
        den[...] = jnp.zeros_like(den)

    @pl.when(first <= offset + tok_rows - 1)
    def _():
        latent = lat_ref[:, :latent_dim]
        rot_key = lat_ref[:, latent_dim:]
        keys = jnp.dot(latent, wk_ref[...], preferred_element_type=jnp.float32)
        values = jnp.dot(latent, wv_ref[...], preferred_element_type=jnp.float32).astype(jnp.bfloat16)
        shape = (tok_rows, block_rows)
        visible = offset + lax.broadcasted_iota(jnp.int32, shape, 0) >= first + lax.broadcasted_iota(
            jnp.int32, shape, 1
        )
        across = (((1,), (1,)), ((), ()))
        for head in range(heads):
            key = keys[:, head * nope_dim : (head + 1) * nope_dim]
            key = rms_norm(key, kg_ref[...]).astype(jnp.bfloat16)
            scores = lax.dot_general(qn_ref[head], key, across, preferred_element_type=jnp.float32)
            scores = scores + lax.dot_general(
                qr_ref[head], rot_key, across, preferred_element_type=jnp.float32
            )
            weights = jnp.where(visible, jnp.exp(scores * scale), 0.0)
            den[head] += jnp.sum(weights, axis=-1, keepdims=True)
            acc[head] += jnp.dot(
                weights.astype(jnp.bfloat16),
                values[:, head * value_dim : (head + 1) * value_dim],
                preferred_element_type=jnp.float32,
            )

    @pl.when(block == pl.num_programs(0) - 1)
    def _():
        for head in range(heads):
            mixed = rms_norm(acc[head] / den[head], og_ref[...])
            out_ref[:, head * value_dim : (head + 1) * value_dim] = mixed.astype(jnp.bfloat16)


def attend(lat_rows, w_key_up, w_value_up, query_nope, query_rope, key_gain, out_gain):
    heads, tok_rows, nope_dim = query_nope.shape
    rope_dim = query_rope.shape[2]
    value_dim = out_gain.shape[0]
    total, width = lat_rows.shape
    block_rows = math.gcd(total, 512)
    whole = pl.BlockSpec(memory_space=VMEM)
    return pl.pallas_call(
        functools.partial(
            attend_kernel, heads, nope_dim, value_dim, width - rope_dim, (nope_dim + rope_dim) ** (-0.5)
        ),
        grid=(total // block_rows,),
        out_shape=jax.ShapeDtypeStruct((tok_rows, heads * value_dim), jnp.bfloat16),
        in_specs=[pl.BlockSpec((block_rows, width), lambda b: (b, 0))] + [whole] * 6,
        out_specs=pl.BlockSpec((tok_rows, heads * value_dim), lambda b: (0, 0)),
        scratch_shapes=[
            VMEM((heads, tok_rows, value_dim), jnp.float32),
            VMEM((heads, tok_rows, 1), jnp.float32),
        ],
        name="attend",
    )(
        lat_rows, w_key_up, w_value_up, query_nope, query_rope,
        key_gain.reshape(1, -1), out_gain.reshape(1, -1),
    )


def on_device(
    queries,
    kv_latent,
    rope_key,
    latent_gain,
    w_key_up,
    w_value_up,
    query_gain,
    key_gain,
    rope_gain,
    out_gain,
    moe_tokens,
    moe_gain,
    routes,
    route_weights,
    w_gate,
    w_up,
    w_down,
):
    quarters = lax.axis_size("tp")
    n_ep = lax.axis_size("ep")
    my_part = lax.axis_index("tp")
    tok_rows = queries.shape[0]
    nope_dim = key_gain.shape[0]
    value_dim = out_gain.shape[0]
    rope_dim = rope_key.shape[1]
    head_count = w_key_up.shape[1] // nope_dim
    positions = lax.axis_index("ep") * tok_rows + jnp.arange(tok_rows, dtype=jnp.int32)
    rot_cos, rot_sin = rope_tables(positions, rope_dim)
    lat_part = tok_rows // quarters

    def mine(values, rows):
        return lax.dynamic_slice_in_dim(values, my_part * rows, rows, 0)

    latent = rms_norm(mine(kv_latent, lat_part).astype(jnp.float32), latent_gain)
    rot_key = rotate(
        rms_norm(mine(rope_key, lat_part).astype(jnp.float32), rope_gain),
        mine(rot_cos, lat_part),
        mine(rot_sin, lat_part),
    )
    lat_own = jnp.concatenate([latent.astype(jnp.bfloat16), rot_key.astype(jnp.bfloat16)], axis=1)

    n_rows, model_dim = moe_tokens.shape
    top_count = routes.shape[1]
    part_rows = n_rows // quarters
    experts = n_ep * w_gate.shape[0]
    capacity = (3 * top_count * part_rows + 2 * experts - 1) // (2 * experts)
    slot_count = experts * capacity
    own_rows = rms_norm(mine(moe_tokens, part_rows).astype(jnp.float32), moe_gain).astype(jnp.bfloat16)
    chosen = mine(routes, part_rows).reshape(part_rows * top_count)
    onehot = (chosen[:, None] == jnp.arange(experts, dtype=jnp.int32)).astype(jnp.float32)
    count = part_rows * top_count
    earlier = (jnp.arange(count)[:, None] > jnp.arange(count)[None, :]).astype(jnp.float32)
    rank = jnp.sum(jnp.dot(earlier, onehot) * onehot, axis=-1).astype(jnp.int32)
    slots = chosen * capacity + rank
    mine_hit = (slots[:, None] == jnp.arange(slot_count, dtype=jnp.int32)).astype(jnp.bfloat16)
    mine_hit = mine_hit.reshape(part_rows, top_count, slot_count)
    outgoing = jnp.einsum(
        "rs,rd->sd", jnp.sum(mine_hit, axis=1), own_rows, preferred_element_type=jnp.float32
    )
    outgoing = outgoing.astype(jnp.bfloat16).reshape(experts, capacity, model_dim)

    arrived, lat_all = spread(outgoing, lat_own, quarters)
    lat_rows = jnp.transpose(lat_all, (2, 1, 0, 3, 4)).reshape(n_ep * tok_rows, lat_own.shape[1])

    shape = arrived.shape
    gate = jnp.einsum("abecd,df->abecf", arrived, w_gate[0], preferred_element_type=jnp.float32)
    upward = jnp.einsum("abecd,df->abecf", arrived, w_up[0], preferred_element_type=jnp.float32)
    hidden = (jax.nn.silu(gate) * upward).astype(jnp.bfloat16)
    partial = jnp.einsum("abecf,fd->aebcd", hidden, w_down[0], preferred_element_type=jnp.float32)
    returned = collect(partial.astype(jnp.bfloat16))

    query = rms_norm(
        queries.astype(jnp.float32).reshape(tok_rows, head_count, nope_dim + rope_dim), query_gain
    )
    query_nope = query[..., :nope_dim].astype(jnp.bfloat16)
    query_rope = rotate(query[..., nope_dim:], rot_cos[:, None, :], rot_sin[:, None, :]).astype(
        jnp.bfloat16
    )
    attended = attend(
        lat_rows,
        w_key_up,
        w_value_up,
        jnp.transpose(query_nope, (1, 0, 2)),
        jnp.transpose(query_rope, (1, 0, 2)),
        key_gain,
        out_gain,
    )

    picked = jnp.einsum(
        "rks,sd->rkd",
        mine_hit,
        returned.reshape(slot_count, model_dim),
        preferred_element_type=jnp.float32,
    )
    own_weights = mine(route_weights, part_rows)
    moe_out = jnp.sum(picked * own_weights[:, :, None], axis=1).astype(jnp.bfloat16)
    return (attended, moe_out)


def solution(mesh):
    return jax.shard_map(
        on_device,
        mesh=mesh,
        in_specs=(
            P("ep", "tp"),
            P("ep", None),
            P("ep", None),
            P(),
            P(None, "tp"),
            P(None, "tp"),
            P(),
            P(),
            P(),
            P(),
            P("ep", None),
            P(),
            P("ep", None),
            P("ep", None),
            P("ep", None, "tp"),
            P("ep", None, "tp"),
            P("ep", "tp", None),
        ),
        out_specs=(P("ep", "tp"), P(("ep", "tp"), None)),
        check_vma=False,
    )
```

```python
import functools
import math

import jax
import jax.numpy as jnp
from jax import lax
from jax.experimental import pallas as pl
from jax.experimental.pallas import tpu as pltpu
from jax.sharding import PartitionSpec as P

EPS = 1e-06
THETA = 500000.0


def rms_norm(values, norm_gain):
    return values * lax.rsqrt(jnp.mean(values * values, axis=-1, keepdims=True) + EPS) * norm_gain


def rope_tables(positions, rope_dim):
    freqs = 1.0 / THETA ** (jnp.arange(0, rope_dim, 2, dtype=jnp.float32) / rope_dim)
    angles = positions.astype(jnp.float32)[:, None] * freqs[None, :]
    return (jnp.cos(angles), jnp.sin(angles))


def rotate(values, rot_cos, rot_sin):
    half_dim = values.shape[-1] // 2
    first_half = values[..., :half_dim]
    second_half = values[..., half_dim:]
    return jnp.concatenate(
        [
            first_half * rot_cos - second_half * rot_sin,
            second_half * rot_cos + first_half * rot_sin,
        ],
        axis=-1,
    )

MESH = pl.DeviceIdType.MESH
VMEM = pltpu.VMEM


def remote(src, dst, send, recv, device):
    return pltpu.make_async_remote_copy(
        src_ref=src, dst_ref=dst, send_sem=send, recv_sem=recv, device_id=device, device_id_type=MESH
    )


def greet(me, quarter, n_ep, highs):
    high, low = quarter // 2, quarter % 2
    barrier = pltpu.get_barrier_semaphore()

    def hello(device):
        pl.semaphore_signal(barrier, inc=1, device_id=device, device_id_type=MESH)

    def hello_ep(step, carry):
        hello((lax.rem(me + step, n_ep), quarter))
        return carry

    lax.fori_loop(1, n_ep, hello_ep, 0)
    hello((me, high * 2 + 1 - low))
    for step in range(1, highs):
        hello((me, lax.rem(high + step, highs) * 2 + low))
    pl.semaphore_wait(barrier, n_ep - 1 + 1 + highs - 1)


def spread_kernel(
    n_ep, highs, rows_ref, lat_ref, arrived, lat_all,
    own_sem, ep_send, ep_recv, high_send, high_recv, low_send, low_recv,
):
    me, quarter = lax.axis_index("ep"), lax.axis_index("tp")
    high, low = quarter // 2, quarter % 2
    partner = (me, high * 2 + 1 - low)
    greet(me, quarter, n_ep, highs)
    payloads = (
        (lambda j: rows_ref.at[j], lambda c, h, j: arrived.at[c, h, j]),
        (lambda j: lat_ref, lambda c, h, j: lat_all.at[j, h, c]),
    )
    own = [
        pltpu.make_async_copy(outgoing(me), into(low, high, me), own_sem.at[p])
        for p, (outgoing, into) in enumerate(payloads)
    ]
    for copy in own:
        copy.start()

    def ep_copy(p, step):
        outgoing, into = payloads[p]
        j = lax.rem(me + step, n_ep)
        return remote(
            outgoing(j), into(low, high, me), ep_send.at[p, step], ep_recv.at[p, step], (j, quarter)
        )

    def ep_arrival(p, step):
        outgoing, into = payloads[p]
        j = lax.rem(me + n_ep - step, n_ep)
        return remote(
            outgoing(me), into(low, high, j), ep_send.at[p, step], ep_recv.at[p, step], (j, quarter)
        )

    def high_copy(p, step, hop):
        into = payloads[p][1]
        j = lax.rem(me + n_ep - step, n_ep)
        block = into(low, high, j)
        return remote(
            block, block, high_send.at[p, hop, step], high_recv.at[p, hop, step],
            (me, lax.rem(high + hop, highs) * 2 + low),
        )

    def high_arrival(p, step, hop):
        into = payloads[p][1]
        j = lax.rem(me + n_ep - step, n_ep)
        block = into(low, lax.rem(high + highs - hop, highs), j)
        return remote(
            block, block, high_send.at[p, hop, step], high_recv.at[p, hop, step],
            (me, lax.rem(high + hop, highs) * 2 + low),
        )

    def low_copy(p, step, hop, side):
        into = payloads[p][1]
        j = lax.rem(me + n_ep - step, n_ep)
        block = into(side, lax.rem(high + highs - hop, highs), j)
        return remote(block, block, low_send.at[p, hop, step], low_recv.at[p, hop, step], partner)

    def start_ep(step, carry, p):
        ep_copy(p, step).start()
        return carry

    def forward(step, carry, p):
        ep_arrival(p, step).wait_recv()
        for hop in range(1, highs):
            high_copy(p, step, hop).start()
        low_copy(p, step, 0, low).start()
        return carry

    def forward_low(step, carry, p):
        for hop in range(1, highs):
            high_arrival(p, step, hop).wait_recv()
            low_copy(p, step, hop, low).start()
        return carry

    def finish(step, carry, p):
        for hop in range(highs):
            low_copy(p, step, hop, 1 - low).wait_recv()
            low_copy(p, step, hop, low).wait_send()
        for hop in range(1, highs):
            high_copy(p, step, hop).wait_send()
        return carry

    def finish_ep(step, carry, p):
        ep_copy(p, step).wait_send()
        return carry

    sent, came = (n_ep, n_ep - me), (n_ep, me + 1)
    for p in range(2):
        lax.fori_loop(1, sent[p], functools.partial(start_ep, p=p), 0)
    for p in range(2):
        own[p].wait()
        for hop in range(1, highs):
            high_copy(p, 0, hop).start()
        low_copy(p, 0, 0, low).start()
        lax.fori_loop(1, came[p], functools.partial(forward, p=p), 0)
    for p in range(2):
        lax.fori_loop(0, came[p], functools.partial(forward_low, p=p), 0)
    for p in range(2):
        lax.fori_loop(0, came[p], functools.partial(finish, p=p), 0)
        lax.fori_loop(1, sent[p], functools.partial(finish_ep, p=p), 0)


def spread(rows, lat, quarters):
    n_ep, cap, model_dim = rows.shape
    highs = quarters // 2
    dma = pltpu.SemaphoreType.DMA
    return pl.pallas_call(
        functools.partial(spread_kernel, n_ep, highs),
        out_shape=(
            jax.ShapeDtypeStruct((2, highs, n_ep, cap, model_dim), rows.dtype),
            jax.ShapeDtypeStruct((n_ep, highs, 2) + lat.shape, lat.dtype),
        ),
        in_specs=[pl.BlockSpec(memory_space=VMEM)] * 2,
        out_specs=(pl.BlockSpec(memory_space=VMEM),) * 2,
        scratch_shapes=[
            dma((2,)),
            dma((2, n_ep)),
            dma((2, n_ep)),
            dma((2, highs, n_ep)),
            dma((2, highs, n_ep)),
            dma((2, highs, n_ep)),
            dma((2, highs, n_ep)),
        ],
        compiler_params=pltpu.CompilerParams(
            collective_id=0, has_side_effects=True, vmem_limit_bytes=60 << 20
        ),
        name="spread",
    )(rows, lat)


def collect_kernel(
    n_ep, highs, part_ref, ret, low_buf, high_buf, sum_buf, final_buf,
    low_send, low_recv, high_send, high_recv, ep_send, ep_recv,
):
    me, quarter = lax.axis_index("ep"), lax.axis_index("tp")
    high, low = quarter // 2, quarter % 2
    partner = (me, high * 2 + 1 - low)
    greet(me, quarter, n_ep, highs)

    def low_copy(step):
        j = lax.rem(me + step, n_ep)
        return remote(
            part_ref.at[1 - low, j], low_buf.at[j], low_send.at[step], low_recv.at[step], partner
        )

    def high_copy(step, hop):
        j = lax.rem(me + step, n_ep)
        other = lax.rem(high + hop, highs)
        return remote(
            sum_buf.at[j, other], high_buf.at[hop, j], high_send.at[hop, step],
            high_recv.at[hop, step], (me, other * 2 + low),
        )

    def ep_copy(step):
        j = lax.rem(me + step, n_ep)
        return remote(final_buf.at[j], ret.at[me], ep_send.at[step], ep_recv.at[step], (j, quarter))

    def ep_arrival(step):
        j = lax.rem(me + n_ep - step, n_ep)
        return remote(final_buf.at[j], ret.at[j], ep_send.at[step], ep_recv.at[step], (j, quarter))

    def start_low(step, carry):
        low_copy(step).start()
        return carry

    def add_low(step, carry):
        low_copy(step).wait_recv()
        j = lax.rem(me + step, n_ep)
        sum_buf[j] = (
            part_ref[low, j].astype(jnp.float32) + low_buf[j].astype(jnp.float32)
        ).astype(jnp.bfloat16)
        for hop in range(1, highs):
            high_copy(step, hop).start()
        return carry

    def total(step):
        j = lax.rem(me + step, n_ep)
        value = part_ref[low, j, high].astype(jnp.float32) + low_buf[j, high].astype(jnp.float32)
        for hop in range(1, highs):
            high_copy(step, hop).wait_recv()
            value = value + high_buf[hop, j].astype(jnp.float32)
        return value.astype(jnp.bfloat16)

    def add_high(step, carry):
        final_buf[lax.rem(me + step, n_ep)] = total(step)
        ep_copy(step).start()
        return carry

    def finish(step, carry):
        ep_arrival(step).wait_recv()
        ep_copy(step).wait_send()
        return carry

    def finish_tp(step, carry):
        low_copy(step).wait_send()
        for hop in range(1, highs):
            high_copy(step, hop).wait_send()
        return carry

    lax.fori_loop(1, n_ep, start_low, 0)
    low_copy(0).start()
    lax.fori_loop(1, n_ep, add_low, 0)
    add_low(0, 0)
    lax.fori_loop(1, n_ep, add_high, 0)
    ret[me] = total(0)
    lax.fori_loop(1, n_ep, finish, 0)
    lax.fori_loop(0, n_ep, finish_tp, 0)


def collect(partial):
    _, n_ep, highs, cap, model_dim = partial.shape
    dma = pltpu.SemaphoreType.DMA
    kind = partial.dtype
    return pl.pallas_call(
        functools.partial(collect_kernel, n_ep, highs),
        out_shape=jax.ShapeDtypeStruct((n_ep, cap, model_dim), kind),
        in_specs=[pl.BlockSpec(memory_space=VMEM)],
        out_specs=pl.BlockSpec(memory_space=VMEM),
        scratch_shapes=[
            VMEM((n_ep, highs, cap, model_dim), kind),
            VMEM((highs, n_ep, cap, model_dim), kind),
            VMEM((n_ep, highs, cap, model_dim), kind),
            VMEM((n_ep, cap, model_dim), kind),
            dma((n_ep,)),
            dma((n_ep,)),
            dma((highs, n_ep)),
            dma((highs, n_ep)),
            dma((n_ep,)),
            dma((n_ep,)),
        ],
        compiler_params=pltpu.CompilerParams(
            collective_id=1, has_side_effects=True, vmem_limit_bytes=62 << 20
        ),
        name="collect",
    )(partial)


def attend_kernel(
    heads, nope_dim, value_dim, latent_dim, scale,
    lat_ref, wk_ref, wv_ref, qn_ref, qr_ref, kg_ref, og_ref, out_ref, acc, den,
):
    block = pl.program_id(0)
    block_rows = lat_ref.shape[0]
    tok_rows = qn_ref.shape[1]
    offset = lax.axis_index("ep") * tok_rows
    first = block * block_rows

    @pl.when(block == 0)
    def _():
        acc[...] = jnp.zeros_like(acc)
        den[...] = jnp.zeros_like(den)

    @pl.when(first <= offset + tok_rows - 1)
    def _():
        latent = lat_ref[:, :latent_dim]
        rot_key = lat_ref[:, latent_dim:]
        keys = jnp.dot(latent, wk_ref[...], preferred_element_type=jnp.float32)
        values = jnp.dot(latent, wv_ref[...], preferred_element_type=jnp.float32).astype(jnp.bfloat16)
        shape = (tok_rows, block_rows)
        visible = offset + lax.broadcasted_iota(jnp.int32, shape, 0) >= first + lax.broadcasted_iota(
            jnp.int32, shape, 1
        )
        across = (((1,), (1,)), ((), ()))
        for head in range(heads):
            key = keys[:, head * nope_dim : (head + 1) * nope_dim]
            key = rms_norm(key, kg_ref[...]).astype(jnp.bfloat16)
            scores = lax.dot_general(qn_ref[head], key, across, preferred_element_type=jnp.float32)
            scores = scores + lax.dot_general(
                qr_ref[head], rot_key, across, preferred_element_type=jnp.float32
            )
            weights = jnp.where(visible, jnp.exp(scores * scale), 0.0)
            den[head] += jnp.sum(weights, axis=-1, keepdims=True)
            acc[head] += jnp.dot(
                weights.astype(jnp.bfloat16),
                values[:, head * value_dim : (head + 1) * value_dim],
                preferred_element_type=jnp.float32,
            )

    @pl.when(block == pl.num_programs(0) - 1)
    def _():
        for head in range(heads):
            mixed = rms_norm(acc[head] / den[head], og_ref[...])
            out_ref[:, head * value_dim : (head + 1) * value_dim] = mixed.astype(jnp.bfloat16)


def attend(lat_rows, w_key_up, w_value_up, query_nope, query_rope, key_gain, out_gain):
    heads, tok_rows, nope_dim = query_nope.shape
    rope_dim = query_rope.shape[2]
    value_dim = out_gain.shape[0]
    total, width = lat_rows.shape
    block_rows = math.gcd(total, tok_rows)
    whole = pl.BlockSpec(memory_space=VMEM)
    return pl.pallas_call(
        functools.partial(
            attend_kernel, heads, nope_dim, value_dim, width - rope_dim, (nope_dim + rope_dim) ** (-0.5)
        ),
        grid=(total // block_rows,),
        out_shape=jax.ShapeDtypeStruct((tok_rows, heads * value_dim), jnp.bfloat16),
        in_specs=[pl.BlockSpec((block_rows, width), lambda b: (b, 0))] + [whole] * 6,
        out_specs=pl.BlockSpec((tok_rows, heads * value_dim), lambda b: (0, 0)),
        scratch_shapes=[
            VMEM((heads, tok_rows, value_dim), jnp.float32),
            VMEM((heads, tok_rows, 1), jnp.float32),
        ],
        name="attend",
    )(
        lat_rows, w_key_up, w_value_up, query_nope, query_rope,
        key_gain.reshape(1, -1), out_gain.reshape(1, -1),
    )


def on_device(
    queries,
    kv_latent,
    rope_key,
    latent_gain,
    w_key_up,
    w_value_up,
    query_gain,
    key_gain,
    rope_gain,
    out_gain,
    moe_tokens,
    moe_gain,
    routes,
    route_weights,
    w_gate,
    w_up,
    w_down,
):
    quarters = lax.axis_size("tp")
    n_ep = lax.axis_size("ep")
    my_part = lax.axis_index("tp")
    tok_rows = queries.shape[0]
    nope_dim = key_gain.shape[0]
    value_dim = out_gain.shape[0]
    rope_dim = rope_key.shape[1]
    head_count = w_key_up.shape[1] // nope_dim
    positions = lax.axis_index("ep") * tok_rows + jnp.arange(tok_rows, dtype=jnp.int32)
    rot_cos, rot_sin = rope_tables(positions, rope_dim)
    lat_part = tok_rows // quarters

    def mine(values, rows):
        return lax.dynamic_slice_in_dim(values, my_part * rows, rows, 0)

    latent = rms_norm(mine(kv_latent, lat_part).astype(jnp.float32), latent_gain)
    rot_key = rotate(
        rms_norm(mine(rope_key, lat_part).astype(jnp.float32), rope_gain),
        mine(rot_cos, lat_part),
        mine(rot_sin, lat_part),
    )
    lat_own = jnp.concatenate([latent.astype(jnp.bfloat16), rot_key.astype(jnp.bfloat16)], axis=1)

    n_rows, model_dim = moe_tokens.shape
    top_count = routes.shape[1]
    part_rows = n_rows // quarters
    experts = n_ep * w_gate.shape[0]
    capacity = (3 * top_count * part_rows + 2 * experts - 1) // (2 * experts)
    slot_count = experts * capacity
    own_rows = rms_norm(mine(moe_tokens, part_rows).astype(jnp.float32), moe_gain).astype(jnp.bfloat16)
    chosen = mine(routes, part_rows).reshape(part_rows * top_count)
    onehot = (chosen[:, None] == jnp.arange(experts, dtype=jnp.int32)).astype(jnp.float32)
    count = part_rows * top_count
    earlier = (jnp.arange(count)[:, None] > jnp.arange(count)[None, :]).astype(jnp.float32)
    rank = jnp.sum(jnp.dot(earlier, onehot) * onehot, axis=-1).astype(jnp.int32)
    slots = chosen * capacity + rank
    mine_hit = (slots[:, None] == jnp.arange(slot_count, dtype=jnp.int32)).astype(jnp.bfloat16)
    mine_hit = mine_hit.reshape(part_rows, top_count, slot_count)
    outgoing = jnp.einsum(
        "rs,rd->sd", jnp.sum(mine_hit, axis=1), own_rows, preferred_element_type=jnp.float32
    )
    outgoing = outgoing.astype(jnp.bfloat16).reshape(experts, capacity, model_dim)

    arrived, lat_all = spread(outgoing, lat_own, quarters)
    lat_rows = lat_all.reshape(n_ep * tok_rows, lat_own.shape[1])

    shape = arrived.shape
    gate = jnp.einsum("abecd,df->abecf", arrived, w_gate[0], preferred_element_type=jnp.float32)
    upward = jnp.einsum("abecd,df->abecf", arrived, w_up[0], preferred_element_type=jnp.float32)
    hidden = (jax.nn.silu(gate) * upward).astype(jnp.bfloat16)
    partial = jnp.einsum("abecf,fd->aebcd", hidden, w_down[0], preferred_element_type=jnp.float32)
    returned = collect(partial.astype(jnp.bfloat16))

    query = rms_norm(
        queries.astype(jnp.float32).reshape(tok_rows, head_count, nope_dim + rope_dim), query_gain
    )
    query_nope = query[..., :nope_dim].astype(jnp.bfloat16)
    query_rope = rotate(query[..., nope_dim:], rot_cos[:, None, :], rot_sin[:, None, :]).astype(
        jnp.bfloat16
    )
    attended = attend(
        lat_rows,
        w_key_up,
        w_value_up,
        jnp.transpose(query_nope, (1, 0, 2)),
        jnp.transpose(query_rope, (1, 0, 2)),
        key_gain,
        out_gain,
    )

    picked = jnp.einsum(
        "rks,sd->rkd",
        mine_hit,
        returned.reshape(slot_count, model_dim),
        preferred_element_type=jnp.float32,
    )
    own_weights = mine(route_weights, part_rows)
    moe_out = jnp.sum(picked * own_weights[:, :, None], axis=1).astype(jnp.bfloat16)
    return (attended, moe_out)


def solution(mesh):
    return jax.shard_map(
        on_device,
        mesh=mesh,
        in_specs=(
            P("ep", "tp"),
            P("ep", None),
            P("ep", None),
            P(),
            P(None, "tp"),
            P(None, "tp"),
            P(),
            P(),
            P(),
            P(),
            P("ep", None),
            P(),
            P("ep", None),
            P("ep", None),
            P("ep", None, "tp"),
            P("ep", None, "tp"),
            P("ep", "tp", None),
        ),
        out_specs=(P("ep", "tp"), P(("ep", "tp"), None)),
        check_vma=False,
    )
```
